32 devices in a mesh: ep: 8 (over z, y), tp: 4 (over x, core).
Axes of the slice: x: 2, y: 2, z: 4, core: 2. Of those that a mesh axis runs over, the one named last changes fastest.
Arguments:
- queries: bfloat16 [8192, 1024], P('ep', 'tp'), may hold values from -6 to 6
- keys: bfloat16 [8192, 1024], P('ep', 'tp'), may hold values from -6 to 6
- values: bfloat16 [8192, 2048], P('ep', 'tp'), may hold values from -6 to 6
- log_input_gate: float32 [8192, 8], P('ep', 'tp'), may hold values from -6 to 103
- forget_preactivation: float32 [8192, 8], P('ep', 'tp'), may hold values from 0 to 16
- forget_offset: float32 [8192, 8], P('ep', 'tp'), may hold values from -0.7 to 0
- head_norm_scale: float32 [2048], P('tp'), may hold values from 0.1 to 1.9
- memory_output_weight: bfloat16 [2048, 4096], P('tp'), may hold values from -0.125 to 0.125
- second_micro_tokens: bfloat16 [4096, 4096], P('ep'), may hold values from -6 to 6
- expert_norm_scale: float32 [4096], replicated, may hold values from 0.1 to 1.9
- expert_choice_index: int32 [4096, 2], P('ep'), may hold values from 0 to 15, all different within a row; in each aligned block of 512 rows (0 to 511, 512 to 1023, ...) at most 96 rows name the same one
- group_likelihood: float32 [4096], P('ep'), may hold values from 0.2 to 1
- expert_raw_weight: float32 [4096, 2], P('ep'), may hold values from 0.1 to 1
- gate_weight: bfloat16 [16, 4096, 1024], P('ep', None, 'tp'), may hold values from -0.09375 to 0.09375
- up_weight: bfloat16 [16, 4096, 1024], P('ep', None, 'tp'), may hold values from -0.09375 to 0.09375
- down_weight: bfloat16 [16, 1024, 4096], P('ep', 'tp'), may hold values from -0.1875 to 0.1875
Outputs:
- mixed: bfloat16 [8192, 4096], P(('ep', 'tp'))
- routed: bfloat16 [4096, 4096], P('ep', 'tp')
The draws below stay inside these ranges and needn't reach their ends.
Inputs may be any that keep to these rules, and one draw needn't show every extreme that they name: `expert_choice_index`: each row names 2 different experts. Within the 512 rows of one index of ep (aligned blocks) no expert is named more than 96 times, and in some blocks one expert is named exactly 96 times.
All inputs are finite; a program needn't handle non-finite values.
Results may differ from the reference program's by a relative error of at most 0.012.
Values may be sent and summed in bfloat16 or wider, within the bound.
A program may use at most 192 MiB of HBM per device.

```python
import math
import jax
import jax.numpy as jnp
import numpy as np
from jax import lax

D = 4096
HEADS = 8
QK = 128
VH = 256
FFE = 1024
TOPK = 2
BLOCK = 128
TA_DEV = 1024
TB_DEV = 512
EXPERTS = 16
TOKA = 8192
TOKB = 4096
CAP = 96
N_EP = 8
N_TP = 4


def draw_log_input_gate(key, part):
    key_one = jax.random.fold_in(key, 0)
    base = -1.5 + 1.5 * jax.random.truncated_normal(key_one, -3.0, 3.0, (TOKA, HEADS), jnp.float32)
    return base


def draw_forget_preactivation(key, part):
    key_one, key_two, key_three, key_four, key_five = jax.random.split(key, 5)
    slow_heads = jax.random.uniform(key_one, (HEADS,), jnp.float32) < 0.5
    jitter = 0.6 * jax.random.truncated_normal(key_four, -2.0, 2.0, (TOKA, HEADS), jnp.float32)
    slow_rate = 0.5 / TOKA * jnp.exp(jax.random.uniform(key_two, (HEADS,), jnp.float32, -0.5, 0.5))
    fast_rate = jnp.exp(jax.random.uniform(key_three, (HEADS,), jnp.float32, math.log(1.0 / 50.0), math.log(1.0 / 30.0)))
    head_rate = jnp.where(slow_heads, slow_rate, fast_rate)
    device_factor = jnp.exp(jax.random.uniform(key_five, (TOKA // TA_DEV, HEADS), jnp.float32, -math.log(2.0), math.log(2.0)))
    device_factor = jnp.repeat(device_factor, TA_DEV, axis=0)
    rate = head_rate[None, :] * device_factor * jnp.exp(jitter)
    return -jnp.log(jnp.expm1(rate))


def draw_forget_offset(key, part):
    key_one, key_two = jax.random.split(key, 2)
    spots = jax.random.randint(key_one, (4,), 0, TOKA)
    struck = jnp.any(jnp.arange(TOKA, dtype=jnp.int32)[:, None] == spots[None, :], axis=1)
    depth = jnp.log(jax.random.uniform(key_two, (TOKA, HEADS), jnp.float32, 0.5, 0.8))
    return jnp.where(struck[:, None], depth, 0.0)


def steps_of(stream_key, extent, shards, least, high):
    def one(dim, blocks):
        draws = jax.random.uniform(jax.random.fold_in(jax.random.fold_in(stream_key, 6), dim), (blocks,), jnp.float32, least / len(shards), high / len(shards))
        return jnp.repeat(jnp.exp(draws), extent[dim] // blocks).reshape((-1,) + (1,) * (len(extent) - dim - 1))

    gain = one(*shards[0])
    for cut in shards[1:]:
        gain = gain * one(*cut)
    return gain


def routed_block(rng, own, number, rows, count, top, most, lean):
    order = jax.random.permutation(rng, count)
    packed, ordinary = portions_of(count, rows * top, most, lean, True), portions_of(count, rows * top, most, lean, False)
    places = jnp.arange(count)

    def named(lengths, turn):
        used = int((lengths > 0).sum())
        fixed = max(1, used // 4)
        shifted = fixed + (places - fixed + turn * (used - fixed)) % max(1, count - fixed)
        return jnp.zeros((count,), jnp.int32).at[order[jnp.where(places < fixed, places, shifted)]].set(jnp.asarray(lengths, jnp.int32))

    lengths = jnp.where(number % 4 == 0, named(packed, number // 4), named(ordinary, number - number // 4 - 1))
    mixed = jax.random.permutation(jax.random.fold_in(own, 3), count)
    donor, sink = mixed[0:count // 2 * 2:2], mixed[1:count // 2 * 2:2]
    margin = jnp.minimum(lengths[donor] - 1, most - lengths[sink]) // 2
    margin = jnp.where((donor == order[0]) | (sink == order[0]) | (lengths[sink] == 0), 0, jnp.maximum(margin, 0))
    shifted = jax.random.randint(jax.random.fold_in(own, 4), (count // 2,), 0, 1 << 20) % (margin + 1)
    lengths = lengths.at[donor].add(-shifted).at[sink].add(shifted)
    members = jnp.searchsorted(jnp.cumsum(lengths), jnp.arange(rows * top), side="right").astype(jnp.int32)
    grid = members.reshape(top, rows).T
    grid = grid[jax.random.permutation(jax.random.fold_in(own, 1), rows)]
    turn = jax.random.randint(jax.random.fold_in(own, 2), (rows, 1), 0, top)
    return jnp.take_along_axis(grid, (jnp.arange(top)[None, :] + turn) % top, axis=1)


def portions_of(count, total, reach, lean, full):
    loads = [(1 << 20) // math.isqrt(standing ** lean) + 1 for standing in range(1, count + 1)]
    largest = reach if full else min(reach, max(-(-total // count), total * loads[0] // sum(loads)))
    least = 1 if total - largest >= count - 1 else 0
    holding, rest = [largest] + [least] * (count - 1), total - largest - least * (count - 1)
    while rest > 0:
        candidates = [i for i in range(1, count) if holding[i] < largest] or [i for i in range(1, count) if holding[i] < reach]
        whole, left = sum([loads[i] for i in candidates]), rest
        for i in candidates:
            extra = min(reach - holding[i], max(1, left * loads[i] // whole), rest)
            holding[i] = holding[i] + extra
            rest = rest - extra
    return np.array(holding)


def noise(own_key, shape, deviation, limit, cuts=(), held_as=jnp.bfloat16):
    entries = deviation * jax.random.normal(own_key, shape, jnp.float32)
    if cuts:
        entries = entries * steps_of(own_key, shape, cuts, -0.22, 0.18)
    return jnp.clip(entries, -limit, limit).astype(held_as)


def setup_inputs(seed: int = 0) -> dict:
    streams_of = jax.random.split(jax.random.key(seed), 17)
    queries = noise(streams_of[0], (TOKA, HEADS * QK), 1.0, 6.0, ((0, 8), (1, 4)))
    keys = noise(streams_of[1], (TOKA, HEADS * QK), 1.0, 6.0, ((0, 8), (1, 4)))
    values = noise(streams_of[2], (TOKA, HEADS * VH), 1.0, 6.0, ((0, 8), (1, 4)))
    log_input_gate = draw_log_input_gate(jax.random.fold_in(streams_of[16], 71), 0)
    forget_preactivation = draw_forget_preactivation(jax.random.fold_in(streams_of[16], 71), 0)
    forget_offset = draw_forget_offset(jax.random.fold_in(streams_of[16], 71), 0)
    head_norm_scale = jnp.clip(1.0 + 0.18 * jax.random.normal(streams_of[6], (HEADS * VH,), jnp.float32), 0.1, 1.9)
    memory_output_weight = noise(streams_of[7], (HEADS * VH, D), (HEADS * VH) ** -0.5, 0.125, ((0, 4),))
    second_micro_tokens = noise(streams_of[8], (TOKB, D), 1.0, 6.0, ((0, 8),))
    expert_norm_scale = jnp.clip(1.0 + 0.18 * jax.random.normal(streams_of[9], (D,), jnp.float32), 0.1, 1.9)
    expert_choice_index_keys = jax.random.split(jax.random.fold_in(streams_of[10], 1), TOKB // TB_DEV)
    expert_choice_index_turns = jax.random.permutation(jax.random.fold_in(streams_of[10], 3), TOKB // TB_DEV)
    expert_choice_index = jax.vmap(lambda own, number: routed_block(jax.random.fold_in(streams_of[10], 2), own, number, TB_DEV, EXPERTS, TOPK, CAP, 1))(expert_choice_index_keys, expert_choice_index_turns).reshape((TOKB, TOPK))
    group_likelihood = jnp.clip(0.2 + 0.8 * jax.random.uniform(streams_of[11], (TOKB,), jnp.float32) ** steps_of(streams_of[11], (TOKB,), ((0, 8),), -0.2, 0.2), 0.2, 1.0)
    expert_raw_weight = jnp.clip(jnp.exp(math.log(1.0) - 2.3025851 * jax.random.uniform(streams_of[12], (TOKB, TOPK), jnp.float32) ** steps_of(streams_of[12], (TOKB, TOPK), ((0, 8),), -0.2, 0.2)), 0.1, 1.0)
    gate_weight = noise(streams_of[13], (EXPERTS, D, FFE), D ** -0.5, 0.09375, ((0, 8), (2, 4)))
    up_weight = noise(streams_of[14], (EXPERTS, D, FFE), D ** -0.5, 0.09375, ((0, 8), (2, 4)))
    down_weight = noise(streams_of[15], (EXPERTS, FFE, D), FFE ** -0.5, 0.1875, ((0, 8), (1, 4)))
    return dict(queries=queries, keys=keys, values=values, log_input_gate=log_input_gate, forget_preactivation=forget_preactivation, forget_offset=forget_offset, head_norm_scale=head_norm_scale, memory_output_weight=memory_output_weight, second_micro_tokens=second_micro_tokens, expert_norm_scale=expert_norm_scale, expert_choice_index=expert_choice_index, group_likelihood=group_likelihood, expert_raw_weight=expert_raw_weight, gate_weight=gate_weight, up_weight=up_weight, down_weight=down_weight)


EPSILON = 1e-06
FLOOR_LOG = -1e+30
HIGHEST = lax.Precision.HIGHEST

def memory_block(carry, piece):
    memory, stable_old = carry
    query_block, key_block, value_block, in_gate, forget_log_factor = piece
    query_float = query_block.astype(jnp.float32)
    key_float = key_block.astype(jnp.float32)
    value_float = value_block.astype(jnp.float32)
    qk_scale = 1.0 / math.sqrt(QK)
    raw_scores = jnp.einsum('htd,hsd->hts', query_float, key_float, precision=HIGHEST) * qk_scale
    running = jnp.cumsum(forget_log_factor, axis=-1)
    totals = running[:, -1]
    causal = jnp.tril(jnp.ones((BLOCK, BLOCK), dtype=bool))
    log_weight = jnp.where(causal, running[:, :, None] - running[:, None, :] + in_gate[:, None, :], -jnp.inf)
    carried = running + stable_old[:, None]
    stable = jnp.maximum(carried, lax.optimization_barrier(jnp.max(log_weight, axis=-1)))
    inner = (raw_scores * jnp.exp(log_weight - stable[..., None])).astype(jnp.bfloat16)
    inner = lax.optimization_barrier(inner).astype(jnp.float32)
    outer = jnp.exp(carried - stable)
    memory_half = lax.optimization_barrier(memory.astype(jnp.bfloat16)).astype(jnp.float32)
    state = outer[..., None] * jnp.einsum('htd,hde->hte', query_float, memory_half, precision=HIGHEST)
    state = state + jnp.einsum('hts,hse->hte', inner, value_float, precision=HIGHEST)
    to_end = totals[:, None] - running + in_gate
    block_peak = lax.optimization_barrier(jnp.max(to_end, axis=-1))
    scaled_keys = key_float * qk_scale
    weighted = (scaled_keys * jnp.exp(to_end - block_peak[:, None])[..., None]).astype(jnp.bfloat16)
    weighted = lax.optimization_barrier(weighted).astype(jnp.float32)
    update = jnp.einsum('hsd,hse->hde', weighted, value_float, precision=HIGHEST)
    stable_new = jnp.maximum(totals + stable_old, block_peak)
    memory = jnp.exp(totals + stable_old - stable_new)[:, None, None] * memory + jnp.exp(block_peak - stable_new)[:, None, None] * update
    return ((memory, stable_new), state)

def recurrence_baseline(queries, keys, values, log_input_gate, forget_preactivation, forget_offset, head_norm_scale, memory_output_weight):
    block_count = TOKA // BLOCK

    def to_blocks(array, width):
        return array.reshape(block_count, BLOCK, HEADS, width).transpose(0, 2, 1, 3)
    forget_log_factor = jax.nn.log_sigmoid(forget_preactivation) + forget_offset
    gate_blocks = log_input_gate.reshape(block_count, BLOCK, HEADS).transpose(0, 2, 1)
    forget_blocks = forget_log_factor.reshape(block_count, BLOCK, HEADS).transpose(0, 2, 1)
    start = (jnp.zeros((HEADS, QK, VH), jnp.float32), jnp.full((HEADS,), FLOOR_LOG, jnp.float32))
    unused, states = lax.scan(memory_block, start, (to_blocks(queries, QK), to_blocks(keys, QK), to_blocks(values, VH), gate_blocks, forget_blocks))
    states = states * lax.rsqrt(lax.optimization_barrier(jnp.mean(states * states, axis=-1, keepdims=True)) + EPSILON)
    hidden = states.transpose(0, 2, 1, 3).reshape(TOKA, HEADS * VH)
    hidden = (hidden * head_norm_scale).astype(jnp.bfloat16)
    group_width = HEADS // N_TP * VH
    total = jnp.zeros((TOKA, D), jnp.float32)
    for group in range(N_TP):
        part = jnp.dot(hidden[:, group * group_width:(group + 1) * group_width], memory_output_weight[group * group_width:(group + 1) * group_width], preferred_element_type=jnp.float32).astype(jnp.bfloat16)
        part = lax.optimization_barrier(part)
        total = total + part.astype(jnp.float32)
    return total.astype(jnp.bfloat16)

def expert_reference(second_micro_tokens, expert_norm_scale, expert_choice_index, group_likelihood, expert_raw_weight, gate_weight, up_weight, down_weight):
    token_float = second_micro_tokens.astype(jnp.float32)
    normed = token_float * lax.rsqrt(lax.optimization_barrier(jnp.mean(token_float * token_float, axis=-1, keepdims=True)) + EPSILON)
    normed = (normed * expert_norm_scale).astype(jnp.bfloat16)
    share = expert_raw_weight / lax.optimization_barrier(jnp.sum(expert_raw_weight, axis=1, keepdims=True))
    route_weight = group_likelihood[:, None] * share
    slot_limit = N_EP * CAP
    unit_width = FFE // N_TP

    def one_expert(total, expert):
        chosen = expert_choice_index == expert
        row_hit = jnp.any(chosen, axis=1)
        row_weight = lax.optimization_barrier(jnp.sum(jnp.where(chosen, route_weight, 0.0), axis=1))
        picked = jnp.nonzero(row_hit, size=slot_limit, fill_value=0)[0].astype(jnp.int32)
        live = (jnp.arange(slot_limit, dtype=jnp.int32) < jnp.sum(row_hit.astype(jnp.int32))).astype(jnp.float32)
        gathered = normed[picked]
        gate = jnp.dot(gathered, gate_weight[expert], preferred_element_type=jnp.float32)
        upward = jnp.dot(gathered, up_weight[expert], preferred_element_type=jnp.float32)
        hidden = (jax.nn.silu(gate) * upward).astype(jnp.bfloat16)
        down = down_weight[expert]
        summed = jnp.zeros((slot_limit, D), jnp.float32)
        for group in range(N_TP):
            part = jnp.dot(hidden[:, group * unit_width:(group + 1) * unit_width], down[group * unit_width:(group + 1) * unit_width], preferred_element_type=jnp.float32).astype(jnp.bfloat16)
            part = lax.optimization_barrier(part)
            summed = summed + part.astype(jnp.float32)
        expert_out = lax.optimization_barrier(summed.astype(jnp.bfloat16))
        contrib = expert_out.astype(jnp.float32) * (row_weight[picked] * live)[:, None]
        return (total.at[picked].add(contrib), None)
    total, unused = lax.scan(one_expert, jnp.zeros((TOKB, D), jnp.float32), jnp.arange(EXPERTS, dtype=jnp.int32))
    return total.astype(jnp.bfloat16)

def reference(queries, keys, values, log_input_gate, forget_preactivation, forget_offset, head_norm_scale, memory_output_weight, second_micro_tokens, expert_norm_scale, expert_choice_index, group_likelihood, expert_raw_weight, gate_weight, up_weight, down_weight):
    mixed = recurrence_baseline(queries, keys, values, log_input_gate, forget_preactivation, forget_offset, head_norm_scale, memory_output_weight)
    routed = expert_reference(second_micro_tokens, expert_norm_scale, expert_choice_index, group_likelihood, expert_raw_weight, gate_weight, up_weight, down_weight)
    return (mixed, routed)
```

```python
import math

import jax
import jax.numpy as jnp
from jax import lax
from jax.sharding import PartitionSpec as P

BLOCK = 128


EPSILON = 1e-06
FLOOR_LOG = -1e30


def rotate(value, axis, step):
    count = lax.axis_size(axis)
    return lax.ppermute(value, axis, [(i, (i + step) % count) for i in range(count)])


def exchange(value, axis, mask):
    count = lax.axis_size(axis)
    return lax.ppermute(value, axis, [(i, i ^ mask) for i in range(count)])


def carried_in(value, axis):
    count, mine = (lax.axis_size(axis), lax.axis_index(axis))
    memory, stable, total = value
    head_count, key_width, value_width = memory.shape
    inclusive = value
    exclusive = (
        jnp.zeros_like(memory),
        jnp.full_like(stable, FLOOR_LOG),
        jnp.zeros_like(total),
    )
    step = 1
    while step < count:
        packed = jnp.concatenate(
            [
                inclusive[0],
                jnp.broadcast_to(inclusive[1][:, None, None], (head_count, 4, value_width)),
                jnp.broadcast_to(inclusive[2][:, None, None], (head_count, 4, value_width)),
            ],
            axis=1,
        )
        packed = lax.ppermute(packed, axis, [(i, i + step) for i in range(count - step)])
        has = mine >= step
        received = (
            packed[:, :key_width],
            jnp.where(has, packed[:, key_width, 0], FLOOR_LOG),
            packed[:, key_width + 4, 0],
        )
        exclusive = merge_states(received, exclusive)
        if 2 * step < count:
            inclusive = merge_states(received, inclusive)
        step *= 2
    return exclusive


def merge_states(earlier, later):
    memory_one, stable_one, total_one = earlier
    memory_two, stable_two, total_two = later
    highest = jnp.maximum(total_two + stable_one, stable_two)
    weight_one = jnp.exp(total_two + stable_one - highest)
    weight_two = jnp.exp(stable_two - highest)
    memory = weight_one[..., None, None] * memory_one + weight_two[..., None, None] * memory_two
    return (memory, highest, total_one + total_two)


def advance(carry, piece):
    return (merge_states(carry, piece), carry)


def recurrence_portion(
    queries,
    keys,
    values,
    log_input_gate,
    forget_preactivation,
    forget_offset,
    head_norm_scale,
    memory_output_weight,
):
    row_count, head_count = log_input_gate.shape
    key_width = queries.shape[1] // head_count
    value_width = values.shape[1] // head_count
    block_count = row_count // BLOCK
    qk_scale = 1.0 / math.sqrt(key_width)
    query_blocks = queries.reshape(block_count, BLOCK, head_count, key_width)
    key_blocks = keys.reshape(block_count, BLOCK, head_count, key_width)
    value_blocks = values.reshape(block_count, BLOCK, head_count, value_width)
    key_float = key_blocks.astype(jnp.float32) * qk_scale
    forget_log_factor = jax.nn.log_sigmoid(forget_preactivation) + forget_offset
    forget_log_factor = forget_log_factor.reshape(block_count, BLOCK, head_count).transpose(0, 2, 1)
    in_gate = log_input_gate.reshape(block_count, BLOCK, head_count).transpose(0, 2, 1)
    running = jnp.cumsum(forget_log_factor, axis=-1)
    totals = running[..., -1]
    to_end = totals[..., None] - running + in_gate
    block_peak = jnp.max(to_end, axis=-1)
    key_weight = jnp.exp(to_end - block_peak[..., None])
    weighted_keys = (key_float * key_weight.transpose(0, 2, 1)[..., None]).astype(jnp.bfloat16)
    block_memory = jnp.einsum(
        "bshd,bshe->bhde", weighted_keys, value_blocks, preferred_element_type=jnp.float32
    )
    empty = (
        jnp.zeros((head_count, key_width, value_width), jnp.float32),
        jnp.full((head_count,), FLOOR_LOG, jnp.float32),
        jnp.zeros((head_count,), jnp.float32),
    )
    device_state, starts = lax.scan(advance, empty, (block_memory, block_peak, totals))
    incoming = carried_in(device_state, "ep")
    memory, peak, unused = merge_states(incoming, starts)
    scores = (
        jnp.einsum("bthd,bshd->bhts", query_blocks, key_blocks, preferred_element_type=jnp.float32)
        * qk_scale
    )
    causal = jnp.tril(jnp.ones((BLOCK, BLOCK), dtype=bool))
    log_weight = running[..., :, None] - running[..., None, :] + in_gate[..., None, :]
    log_weight = jnp.where(causal, log_weight, -jnp.inf)
    carried = running + peak[..., None]
    stable = jnp.maximum(carried, jnp.max(log_weight, axis=-1))
    inner = (scores * jnp.exp(log_weight - stable[..., None])).astype(jnp.bfloat16)
    outer = jnp.exp(carried - stable)
    memory_half = memory.astype(jnp.bfloat16)
    state = outer[..., None] * jnp.einsum(
        "bthd,bhde->bhte", query_blocks, memory_half, preferred_element_type=jnp.float32
    )
    state = state + jnp.einsum(
        "bhts,bshe->bhte", inner, value_blocks, preferred_element_type=jnp.float32
    )
    state = state * lax.rsqrt(jnp.mean(state * state, axis=-1, keepdims=True) + EPSILON)
    hidden = state.transpose(0, 2, 1, 3).reshape(row_count, head_count * value_width)
    hidden = (hidden * head_norm_scale).astype(jnp.bfloat16)
    tp_size, me = lax.axis_size("tp"), lax.axis_index("tp")
    rows = row_count // tp_size
    part = jnp.dot(hidden, memory_output_weight, preferred_element_type=jnp.float32)
    part = part.astype(jnp.bfloat16).reshape(tp_size, rows, -1)
    held = {mask: lax.dynamic_index_in_dim(part, me ^ mask, 0, False) for mask in range(tp_size)}
    bit = 1
    while bit < tp_size:
        keep = {mask: block for mask, block in held.items() if not mask & bit}
        for mask in keep:
            arrived = exchange(held[mask | bit], "tp", bit)
            keep[mask] = (
                keep[mask].astype(jnp.float32) + arrived.astype(jnp.float32)
            ).astype(jnp.bfloat16)
        held = keep
        bit *= 2
    return held[0]


def expert_half(
    second_micro_tokens,
    expert_norm_scale,
    expert_choice_index,
    group_likelihood,
    expert_raw_weight,
    gate_weight,
    up_weight,
    down_weight,
):
    token_count, model_width = second_micro_tokens.shape
    pick_count = expert_choice_index.shape[1]
    local_experts = gate_weight.shape[0]
    ep_size = lax.axis_size("ep")
    tp_size = lax.axis_size("tp")
    expert_count = local_experts * ep_size
    capacity = tp_size * max(1, 3 * pick_count * token_count // (2 * expert_count * tp_size))
    token_float = second_micro_tokens.astype(jnp.float32)
    normed = token_float * lax.rsqrt(
        jnp.mean(token_float * token_float, axis=-1, keepdims=True) + EPSILON
    )
    normed = (normed * expert_norm_scale).astype(jnp.bfloat16)
    share = expert_raw_weight / jnp.sum(expert_raw_weight, axis=1, keepdims=True)
    route_weight = group_likelihood[:, None] * share
    me, mine = lax.axis_index("ep"), lax.axis_index("tp")
    hidden_units, out_width = down_weight.shape[1:]
    columns = out_width // tp_size

    def weight_for(mask):
        return lax.dynamic_slice_in_dim(down_weight, (mine ^ mask) * columns, columns, 2)

    down_pieces = [weight_for(0)]
    for mask in range(1, tp_size):
        down_pieces.append(exchange(weight_for(mask), "tp", mask))
    down_columns = jnp.concatenate(down_pieces, axis=1)

    quarter = capacity // tp_size
    experts = jnp.arange(expert_count, dtype=jnp.int32)
    named = expert_choice_index[:, :, None] == experts
    named_token = jnp.sum(named.astype(jnp.float32), axis=1)
    earlier = jnp.tril(jnp.ones((token_count, token_count), jnp.bfloat16), -1)
    before = jnp.dot(
        earlier, named_token.astype(jnp.bfloat16), preferred_element_type=jnp.float32
    )
    slot_rank = jnp.sum(jnp.where(named, before[:, None, :], 0.0), axis=2).astype(jnp.int32)
    slot_index = expert_choice_index * capacity + slot_rank

    def owner_of(step):
        return lax.rem(me + step, ep_size)

    send_shape = (ep_size, local_experts, quarter)
    step, expert, row = (lax.broadcasted_iota(jnp.int32, send_shape, i) for i in range(3))
    send_slot = (
        (owner_of(step) * local_experts + expert) * capacity + mine * quarter + row
    ).reshape(-1)
    chosen = send_slot[:, None] == slot_index[:, 0][None, :]
    for pick in range(1, pick_count):
        chosen = chosen | (send_slot[:, None] == slot_index[:, pick][None, :])
    outgoing = jnp.dot(
        chosen.astype(jnp.bfloat16), normed, preferred_element_type=jnp.float32
    ).astype(jnp.bfloat16)
    outgoing = outgoing.reshape(ep_size, local_experts, quarter, model_width)
    arrived = [outgoing[0]] + [rotate(outgoing[k], "ep", k) for k in range(1, ep_size)]

    rows = {0: jnp.concatenate(arrived, axis=1)}
    bit = tp_size // 2
    while bit:
        for place in list(rows):
            rows[place | bit] = exchange(rows[place], "tp", bit)
        bit //= 2

    def hidden_of(block):
        gate = jnp.einsum("erd,edf->erf", block, gate_weight, preferred_element_type=jnp.float32)
        upward = jnp.einsum("erd,edf->erf", block, up_weight, preferred_element_type=jnp.float32)
        return (jax.nn.silu(gate) * upward).astype(jnp.bfloat16)

    row_count = ep_size * quarter
    half = max(1, tp_size // 2)
    hidden = []
    for first in range(0, tp_size, half):
        block = jnp.concatenate([rows[place] for place in range(first, first + half)], axis=1)
        hidden.append(hidden_of(block))
    hidden = jnp.concatenate(hidden, axis=1)
    hidden = hidden.reshape(local_experts, tp_size, row_count, hidden_units)
    units = {0: hidden}
    bit = tp_size // 2
    while bit:
        for mask in list(units):
            units[mask | bit] = exchange(units[mask], "tp", bit)
        bit //= 2
    full_hidden = jnp.concatenate(
        [
            jnp.stack([units[mask][:, place ^ mask] for place in range(tp_size)], axis=1)
            for mask in range(tp_size)
        ],
        axis=3,
    ).reshape(local_experts, tp_size * row_count, tp_size * hidden_units)
    result = jnp.einsum(
        "erf,efc->erc", full_hidden, down_columns, preferred_element_type=jnp.float32
    ).astype(jnp.bfloat16)
    result = result.reshape(local_experts, tp_size, ep_size, quarter, columns)
    returned = [result[:, :, 0]]
    returned += [rotate(result[:, :, k], "ep", -k) for k in range(1, ep_size)]
    returned = jnp.stack(returned).reshape(-1, columns)

    back_shape = (ep_size, local_experts, tp_size, quarter)
    step, expert, place, row = (lax.broadcasted_iota(jnp.int32, back_shape, i) for i in range(4))
    back_slot = (
        (owner_of(step) * local_experts + expert) * capacity + (mine ^ place) * quarter + row
    ).reshape(-1)
    spread = jnp.zeros((token_count, back_slot.shape[0]), jnp.float32)
    for pick in range(pick_count):
        spread = spread + jnp.where(
            slot_index[:, pick : pick + 1] == back_slot[None, :],
            route_weight[:, pick : pick + 1],
            0.0,
        )
    spread_high = spread.astype(jnp.bfloat16)
    spread_low = (spread - spread_high.astype(jnp.float32)).astype(jnp.bfloat16)
    combined = jnp.dot(spread_high, returned, preferred_element_type=jnp.float32) + jnp.dot(
        spread_low, returned, preferred_element_type=jnp.float32
    )
    return combined.astype(jnp.bfloat16)


def per_device(
    queries,
    keys,
    values,
    log_input_gate,
    forget_preactivation,
    forget_offset,
    head_norm_scale,
    memory_output_weight,
    second_micro_tokens,
    expert_norm_scale,
    expert_choice_index,
    group_likelihood,
    expert_raw_weight,
    gate_weight,
    up_weight,
    down_weight,
):
    mixed = recurrence_portion(
        queries,
        keys,
        values,
        log_input_gate,
        forget_preactivation,
        forget_offset,
        head_norm_scale,
        memory_output_weight,
    )
    routed = expert_half(
        second_micro_tokens,
        expert_norm_scale,
        expert_choice_index,
        group_likelihood,
        expert_raw_weight,
        gate_weight,
        up_weight,
        down_weight,
    )
    return (mixed, routed)


def solution(mesh):
    in_specs = (
        P("ep", "tp"),
        P("ep", "tp"),
        P("ep", "tp"),
        P("ep", "tp"),
        P("ep", "tp"),
        P("ep", "tp"),
        P("tp"),
        P("tp", None),
        P("ep", None),
        P(),
        P("ep", None),
        P("ep"),
        P("ep", None),
        P("ep", None, "tp"),
        P("ep", None, "tp"),
        P("ep", "tp", None),
    )
    out_specs = (P(("ep", "tp"), None), P("ep", "tp"))
    return jax.shard_map(
        per_device, mesh=mesh, in_specs=in_specs, out_specs=out_specs, check_vma=False
    )
```
